32 devices in a mesh: sp: 8 (over z, y), tp: 4 (over x, core).
Axes of the slice: x: 2, y: 2, z: 4, core: 2. Of those that a mesh axis runs over, the one named last changes fastest.
Arguments:
- stream: bfloat16 [2048, 2048], P('sp'), may hold values from -6 to 6
- narrow_query_weight: bfloat16 [2048, 1024], P('sp', 'tp'), may hold values from -6 to 6
- wide_query_weight: bfloat16 [2048, 2048], P('sp', 'tp'), may hold values from -6 to 6
- value_rows_heads: bfloat16 [2048, 2, 1024], P('sp', None, 'tp'), may hold values from -6 to 6
- output_gate_logits: bfloat16 [2048, 2, 1024], P('sp', None, 'tp'), may hold values from -6 to 6
- narrow_forget_logits: bfloat16 [2, 2048, 1024], P(None, 'sp', 'tp'), may hold values from -6 to 6
- wide_forget_logits: bfloat16 [2, 2048, 2048], P(None, 'sp', 'tp'), may hold values from -6 to 6
- narrow_forget_headroom: float32 [2, 1024], P(None, 'tp'), may hold values from 0 to 0.08, as said below
- wide_forget_headroom: float32 [2, 2048], P(None, 'tp'), may hold values from 0 to 0.08, as said below
- extra_log_decay: float32 [2048, 2, 16], P('sp', None, 'tp'), may hold values from -1.4 to 0
- per_head_norm_gain: float32 [64], replicated, may hold values from 0.1 to 1.9
- mixer_output_weight: bfloat16 [2, 1024, 2048], replicated, may hold values from -0.125 to 0.125
- feedforward_norm_gain: float32 [2048], replicated, may hold values from 0.1 to 1.9
- expert_gate_matrix: bfloat16 [8, 2048, 4096], P('sp', None, 'tp'), may hold values from -0.125 to 0.125
- expert_up_matrix: bfloat16 [8, 2048, 4096], P('sp', None, 'tp'), may hold values from -0.125 to 0.125
- expert_down_matrix: bfloat16 [8, 4096, 2048], P('sp', 'tp'), may hold values from -0.09375 to 0.09375
- routes: int32 [2048, 2], P('sp'), may hold values from 0 to 7, all different within a row; in each aligned block of 64 rows (0 to 63, 64 to 127, ...) at most 32 rows name the same one
- router_scores_chosen: float32 [2048, 2], P('sp'), may hold values from -8 to 8
Outputs:
- result: bfloat16 [2048, 2048], P(('sp', 'tp'))
The draws below stay inside these ranges and needn't reach their ends.
Inputs may be any that keep to these rules, and one draw needn't show every extreme that they name: `routes`: each row names 2 different experts; in each aligned block of 64 rows no expert is named by more than 32 rows. `narrow_forget_headroom`: positive. `wide_forget_headroom`: positive.
All inputs are finite; a program needn't handle non-finite values.
Results may differ from the reference program's by a relative error of at most 0.011.
Values may be sent and summed in bfloat16 or wider, within the bound.
A program may use at most 128 MiB of HBM per device.

```python
import math
from functools import partial
import jax
import jax.numpy as jnp
import numpy as np
from jax import lax

D = 2048
HG = 16
DV = 64
DKN = 64
DKW = 128
FF_EXP = 4096
TOP = 2
BLOCK = 64
TOK_DEV = 256
TOKENS = 2048
ROWS = 64
EXPERTS = 8
CAP = 32
N_TP = 4


def forget_field(key, state_rows):
    first_key, second_key = jax.random.split(jax.random.fold_in(key, 17))
    device_spans = TOKENS // TOK_DEV
    full_shape = (2, TOKENS, HG * state_rows)
    offsets = jax.random.uniform(first_key, (2, device_spans, 1), jnp.float32, -1.2, 1.2)
    jitter = jnp.clip(jax.random.normal(second_key, full_shape, jnp.float32), -4.0, 4.0)
    return (jnp.repeat(offsets, TOK_DEV, axis=1) + jitter).astype(jnp.bfloat16)


def room_field(key, state_rows):
    subkeys = jax.random.split(jax.random.fold_in(key, 29), 3)
    quick_share = 0.5
    is_quick = jax.random.bernoulli(subkeys[0], quick_share, (2, HG, 1))
    quick_room = jnp.exp(jax.random.uniform(subkeys[1], (2, HG, state_rows), jnp.float32, jnp.log(0.04), jnp.log(0.08)))
    lasting_room = jax.random.uniform(subkeys[2], (2, HG, state_rows), jnp.float32, 0.2, 0.7) * (2.0 / TOKENS)
    return jnp.where(is_quick, quick_room, lasting_room).reshape(2, HG * state_rows).astype(jnp.float32)


def draw_narrow_forget_logits(key, part):
    return forget_field(key, DKN)


def draw_wide_forget_logits(key, part):
    return forget_field(jax.random.fold_in(key, 5), DKW)


def draw_narrow_forget_headroom(key, part):
    return room_field(key, DKN)


def draw_wide_forget_headroom(key, part):
    return room_field(jax.random.fold_in(key, 7), DKW)


def draw_extra_log_decay(key, part):
    first_key, second_key = jax.random.split(jax.random.fold_in(key, 43))
    positions = jax.random.randint(first_key, (2, 2, HG), 0, TOKENS)
    losses = jnp.log(jax.random.uniform(second_key, (2, 2, HG), jnp.float32, 0.5, 0.8))
    matches = jnp.arange(TOKENS)[:, None, None, None] == positions[None]
    return jnp.sum(jnp.where(matches, losses[None], 0.0), axis=1).astype(jnp.float32)


def levels(rng, extent, shards, smallest, top_value):
    factor_of = 1.0
    for axis_at, parts in shards:
        steps = jax.random.uniform(jax.random.fold_in(jax.random.fold_in(rng, 6), axis_at), (parts,), jnp.float32, smallest / len(shards), top_value / len(shards))
        factor_of = factor_of * jnp.repeat(jnp.exp(steps), extent[axis_at] // parts).reshape((-1,) + (1,) * (len(extent) - 1 - axis_at))
    return factor_of


def routed_block(rng, own, number, rows, number_of, top, reach, skew):
    order = jax.random.permutation(rng, number_of)
    heavy_load, common = shares(number_of, rows * top, reach, skew, True), shares(number_of, rows * top, reach, skew, False)
    places = jnp.arange(number_of)

    def named(lengths, turn):
        used = int((lengths > 0).sum())
        fixed = max(1, used // 4)
        shifted = fixed + (places - fixed + turn * (used - fixed)) % max(1, number_of - fixed)
        return jnp.zeros((number_of,), jnp.int32).at[order[jnp.where(places < fixed, places, shifted)]].set(jnp.asarray(lengths, jnp.int32))

    lengths = jnp.where(number % 4 == 0, named(heavy_load, number // 4), named(common, number - number // 4 - 1))
    mixed = jax.random.permutation(jax.random.fold_in(own, 3), number_of)
    donor, receiver = mixed[0:number_of // 2 * 2:2], mixed[1:number_of // 2 * 2:2]
    room = jnp.minimum(lengths[donor] - 1, reach - lengths[receiver]) // 2
    room = jnp.where((donor == order[0]) | (receiver == order[0]) | (lengths[receiver] == 0), 0, jnp.maximum(room, 0))
    shifted = jax.random.randint(jax.random.fold_in(own, 4), (number_of // 2,), 0, 1 << 20) % (room + 1)
    lengths = lengths.at[donor].add(-shifted).at[receiver].add(shifted)
    labels = jnp.searchsorted(jnp.cumsum(lengths), jnp.arange(rows * top), side="right").astype(jnp.int32)
    grid = labels.reshape(top, rows).T
    grid = grid[jax.random.permutation(jax.random.fold_in(own, 1), rows)]
    turn = jax.random.randint(jax.random.fold_in(own, 2), (rows, 1), 0, top)
    return jnp.take_along_axis(grid, (jnp.arange(top)[None, :] + turn) % top, axis=1)


def shares(number_of, total, reach, lean, full):
    loads = [(1 << 20) // math.isqrt(grade ** lean) + 1 for grade in range(1, number_of + 1)]
    largest = reach if full else min(reach, max(-(-total // number_of), total * loads[0] // sum(loads)))
    least = 1 if total - largest >= number_of - 1 else 0
    given, rest = [largest] + [least] * (number_of - 1), total - largest - least * (number_of - 1)
    while rest > 0:
        candidates = [i for i in range(1, number_of) if given[i] < largest] or [i for i in range(1, number_of) if given[i] < reach]
        mass, left = sum([loads[i] for i in candidates]), rest
        for i in candidates:
            extra = min(reach - given[i], max(1, left * loads[i] // mass), rest)
            given[i] = given[i] + extra
            rest = rest - extra
    return np.array(given)


def normal_values(rng, extent, spread, limit, cuts=(), held_as=jnp.bfloat16):
    loudness = levels(rng, extent, cuts, -0.22, 0.18) if cuts else 1.0
    entries = jax.random.normal(rng, extent, jnp.float32) * spread * loudness
    return jnp.minimum(jnp.maximum(entries, -limit), limit).astype(held_as)


def setup_inputs(seed: int = 0) -> dict:
    seeds = jax.random.split(jax.random.key(seed), 19)
    stream = normal_values(seeds[0], (TOKENS, D), 1.0, 6.0, ((0, 8),))
    narrow_query_weight = normal_values(seeds[1], (TOKENS, HG * DKN), 1.0, 6.0, ((0, 8), (1, 4)))
    wide_query_weight = normal_values(seeds[2], (TOKENS, HG * DKW), 1.0, 6.0, ((0, 8), (1, 4)))
    value_rows_heads = normal_values(seeds[3], (TOKENS, 2, HG * DV), 1.0, 6.0, ((0, 8), (2, 4)))
    output_gate_logits = normal_values(seeds[4], (TOKENS, 2, HG * DV), 1.0, 6.0, ((0, 8), (2, 4)))
    narrow_forget_logits = draw_narrow_forget_logits(jax.random.fold_in(seeds[18], 71), 0)
    wide_forget_logits = draw_wide_forget_logits(jax.random.fold_in(seeds[18], 71), 0)
    narrow_forget_headroom = draw_narrow_forget_headroom(jax.random.fold_in(seeds[18], 71), 0)
    wide_forget_headroom = draw_wide_forget_headroom(jax.random.fold_in(seeds[18], 71), 0)
    extra_log_decay = draw_extra_log_decay(jax.random.fold_in(seeds[18], 71), 0)
    per_head_norm_gain = jnp.clip(1.0 + 0.18 * jax.random.normal(seeds[10], (DV,), jnp.float32), 0.1, 1.9)
    mixer_output_weight = normal_values(seeds[11], (2, HG * DV, D), (2 * HG * DV) ** -0.5, 0.125)
    feedforward_norm_gain = jnp.clip(1.0 + 0.18 * jax.random.normal(seeds[12], (D,), jnp.float32), 0.1, 1.9)
    expert_gate_matrix = normal_values(seeds[13], (EXPERTS, D, FF_EXP), D ** -0.5, 0.125, ((0, 8), (2, 4)))
    expert_up_matrix = normal_values(seeds[14], (EXPERTS, D, FF_EXP), D ** -0.5, 0.125, ((0, 8), (2, 4)))
    expert_down_matrix = normal_values(seeds[15], (EXPERTS, FF_EXP, D), FF_EXP ** -0.5, 0.09375, ((0, 8), (1, 4)))
    routes_keys = jax.random.split(jax.random.fold_in(seeds[16], 1), TOKENS // ROWS)
    routes_turns = jax.random.permutation(jax.random.fold_in(seeds[16], 3), TOKENS // ROWS)
    routes = jax.vmap(lambda own, number: routed_block(jax.random.fold_in(seeds[16], 2), own, number, ROWS, EXPERTS, TOP, CAP, 2))(routes_keys, routes_turns).reshape((TOKENS, TOP))
    router_scores_chosen = normal_values(seeds[17], (TOKENS, TOP), 2.0, 8.0, ((0, 8),), jnp.float32)
    return {"stream": stream, "narrow_query_weight": narrow_query_weight, "wide_query_weight": wide_query_weight, "value_rows_heads": value_rows_heads, "output_gate_logits": output_gate_logits, "narrow_forget_logits": narrow_forget_logits, "wide_forget_logits": wide_forget_logits, "narrow_forget_headroom": narrow_forget_headroom, "wide_forget_headroom": wide_forget_headroom, "extra_log_decay": extra_log_decay, "per_head_norm_gain": per_head_norm_gain, "mixer_output_weight": mixer_output_weight, "feedforward_norm_gain": feedforward_norm_gain, "expert_gate_matrix": expert_gate_matrix, "expert_up_matrix": expert_up_matrix, "expert_down_matrix": expert_down_matrix, "routes": routes, "router_scores_chosen": router_scores_chosen}


EPS = 1e-06
TOP_PRECISION = lax.Precision.HIGHEST

def block_sweep(query_rows, block_openings, values, decay_logarithm):
    token_rows, total_head_count, state_rows = query_rows.shape
    value_size = values.shape[2]
    blocks = token_rows // BLOCK

    def to_blocks(source):
        return source.reshape(blocks, BLOCK, total_head_count, source.shape[2]).transpose(0, 2, 1, 3)
    inside = jnp.cumsum(to_blocks(decay_logarithm), axis=2)
    triangle = jnp.tril(jnp.ones((BLOCK, BLOCK), jnp.float32))

    def advance(present_state, inputs):
        block_of_queries, block_opening_state, block_of_values, inside_block = inputs
        ending = inside_block[:, -1:, :]
        query_within_block = block_of_queries * jnp.exp(inside_block)
        k_inside = block_opening_state * jnp.exp(-inside_block)
        key_block_ending = block_opening_state * jnp.exp(ending - inside_block)
        scores = jnp.einsum('htk,hsk->hts', query_within_block, k_inside, precision=TOP_PRECISION) * triangle
        final_output = jnp.einsum('hts,hsv->htv', scores, block_of_values, precision=TOP_PRECISION)
        final_output = final_output + jnp.einsum('ifm,imo->ifo', query_within_block, present_state, precision=TOP_PRECISION)
        expanded_state = jnp.einsum('lbi,lbp->lip', key_block_ending, block_of_values, precision=TOP_PRECISION)
        present_state = present_state * jnp.exp(ending[:, 0, :])[:, :, None] + expanded_state
        return (present_state, final_output)
    zero_state = jnp.zeros((total_head_count, state_rows, value_size), jnp.float32)
    closing_state, outputs = lax.scan(advance, zero_state, (to_blocks(query_rows), to_blocks(block_openings), to_blocks(values), inside))
    return outputs.transpose(0, 2, 1, 3).reshape(token_rows, total_head_count, value_size)

def slot_table(block_routes, experts, capacity):
    flattened = block_routes.reshape(-1)
    matches = (flattened[:, None] == jnp.arange(experts, dtype=jnp.int32)[None, :]).astype(jnp.int32)
    earlier = jnp.cumsum(matches, axis=0) - matches
    token_position = lax.optimization_barrier(jnp.sum(earlier * matches, axis=1)).astype(jnp.int32)
    return (flattened * capacity + token_position).reshape(block_routes.shape)

def reference(stream, narrow_query_weight, wide_query_weight, value_rows_heads, output_gate_logits, narrow_forget_logits, wide_forget_logits, narrow_forget_headroom, wide_forget_headroom, extra_log_decay, per_head_norm_gain, mixer_output_weight, feedforward_norm_gain, expert_gate_matrix, expert_up_matrix, expert_down_matrix, routes, router_scores_chosen):
    groups = ((narrow_query_weight, narrow_forget_logits, narrow_forget_headroom), (wide_query_weight, wide_forget_logits, wide_forget_headroom))
    mixed_groups = []
    for head_group_index in range(2):
        query_rows, forget_gate, forget_headroom = groups[head_group_index]
        query_heads = jax.nn.silu(query_rows.astype(jnp.float32)).reshape(TOKENS, HG, -1)
        value_heads = value_rows_heads[:, head_group_index].astype(jnp.float32).reshape(TOKENS, HG, DV)
        pre_forget = forget_gate.astype(jnp.float32).reshape(2, TOKENS, HG, -1)
        block_openings = jax.nn.sigmoid(-pre_forget) * forget_headroom.reshape(2, 1, HG, -1)
        decay_logarithm = jnp.log1p(-block_openings) + extra_log_decay[None, :, head_group_index, :, None]
        ahead = block_sweep(query_heads, block_openings[0], value_heads, decay_logarithm[0])
        behind = jnp.flip(block_sweep(jnp.flip(query_heads, 0), jnp.flip(block_openings[1], 0), jnp.flip(value_heads, 0), jnp.flip(decay_logarithm[1], 0)), 0)
        summed = ahead + behind
        scale = lax.rsqrt(lax.optimization_barrier(jnp.mean(summed * summed, axis=-1, keepdims=True)) + EPS)
        gates = jax.nn.silu(output_gate_logits[:, head_group_index].astype(jnp.float32)).reshape(TOKENS, HG, DV)
        mixed_groups.append((summed * scale * per_head_norm_gain * gates).reshape(TOKENS, HG * DV))
    mixed = jnp.stack(mixed_groups, axis=1).astype(jnp.bfloat16).reshape(TOKENS, 2 * HG * DV)
    projected = jnp.dot(mixed, mixer_output_weight.reshape(2 * HG * DV, D), preferred_element_type=jnp.float32)
    residual = stream.astype(jnp.float32) + projected
    norm_rows = (residual * lax.rsqrt(lax.optimization_barrier(jnp.mean(residual * residual, axis=-1, keepdims=True)) + EPS) * feedforward_norm_gain).astype(jnp.bfloat16)
    blocks = TOKENS // ROWS
    slot_count = EXPERTS * CAP
    slot_ids = jax.vmap(partial(slot_table, experts=EXPERTS, capacity=CAP))(routes.reshape(blocks, ROWS, TOP))
    global_slots = (slot_ids + (jnp.arange(blocks, dtype=jnp.int32) * slot_count)[:, None, None]).reshape(-1)
    row_ids = jnp.repeat(jnp.arange(TOKENS, dtype=jnp.int32), TOP)
    row_table = jnp.full((blocks * slot_count,), TOKENS, jnp.int32).at[global_slots].set(row_ids)
    row_table = row_table.reshape(blocks, EXPERTS, CAP).transpose(1, 0, 2).reshape(EXPERTS, blocks * CAP)
    padded_rows = jnp.concatenate([norm_rows, jnp.zeros((1, D), jnp.bfloat16)], axis=0)
    quarter_width = FF_EXP // N_TP

    def one_expert(inputs):
        row_index, gate_weights, up_weights, down_weights = inputs
        gathered = padded_rows[row_index]
        gate_part = jnp.dot(gathered, gate_weights, preferred_element_type=jnp.float32)
        up_part = jnp.dot(gathered, up_weights, preferred_element_type=jnp.float32)
        hidden = (jax.nn.silu(gate_part) * up_part).astype(jnp.bfloat16)
        combined = jnp.zeros((gathered.shape[0], D), jnp.float32)
        for quarter in range(N_TP):
            lower_edge = quarter * quarter_width
            upper_edge = lower_edge + quarter_width
            partial_out = jnp.dot(hidden[:, lower_edge:upper_edge], down_weights[lower_edge:upper_edge], preferred_element_type=jnp.float32).astype(jnp.bfloat16)
            combined = combined + lax.optimization_barrier(partial_out).astype(jnp.float32)
        return combined.astype(jnp.bfloat16)
    expert_out = lax.map(one_expert, (row_table, expert_gate_matrix, expert_up_matrix, expert_down_matrix))
    expert_out = expert_out.reshape(EXPERTS, blocks, CAP, D).transpose(1, 0, 2, 3).reshape(blocks * slot_count, D)
    picked = expert_out[global_slots].reshape(TOKENS, TOP, D)
    weights = jax.nn.sigmoid(router_scores_chosen - router_scores_chosen[:, ::-1])
    mixed_out = lax.optimization_barrier(jnp.sum(weights[:, :, None] * picked.astype(jnp.float32), axis=1))
    return (residual + mixed_out).astype(jnp.bfloat16)
```

```python
from functools import partial

import jax
import jax.numpy as jnp
from jax import lax
from jax.experimental import pallas as pl
from jax.experimental.pallas import tpu as pltpu
from jax.sharding import PartitionSpec as P

BLOCK = 64
LANES = 128
EPS = 1e-06
F32 = jnp.float32
BF16 = jnp.bfloat16
MESH = pl.DeviceIdType.MESH
NT = (((1,), (1,)), ((), ()))
TN = (((0,), (0,)), ((), ()))
VMEM = pl.BlockSpec(memory_space=pltpu.VMEM)


def dot(a, b, dims=(((1,), (0,)), ((), ()))):
    return lax.dot_general(a, b, dims, preferred_element_type=F32)


def split_dot(exact, x):
    hi = x.astype(BF16)
    lo = (x - hi.astype(F32)).astype(BF16)
    return dot(exact, hi) + dot(exact, lo)


def tile_list(narrow, wide, heads, value_size):
    tiles = []
    pairs = heads * value_size // LANES
    for j in range(narrow // LANES):
        tiles.append((0, j * LANES, j * LANES, (2 * j, 2 * j + 1), j * LANES, 2))
    for h in range(wide // LANES):
        at = h * LANES
        tiles.append((1, at, narrow + at, (h, h), (pairs + h // 2) * LANES, h % 2))
    return tiles


def state_mask(kind, value_size):
    rows = lax.broadcasted_iota(jnp.int32, (LANES, LANES), 0) // value_size
    cols = lax.broadcasted_iota(jnp.int32, (LANES, LANES), 1) // value_size
    return rows == cols if kind == 2 else rows == kind


def mix_kernel(heads, nq, wq, v, nf, wf, nr, wr, ex, o_ref, run_ref, msg_ref):
    tokens = nq.shape[0]
    value_size = v.shape[1] // (2 * heads)
    blocks = tokens // BLOCK
    row = lax.broadcasted_iota(jnp.int32, (tokens, tokens), 0)
    col = lax.broadcasted_iota(jnp.int32, (tokens, tokens), 1)
    same = (row // BLOCK) == (col // BLOCK)
    wanted = (same & (row >= col), same & (row <= col))
    tri = tuple(jnp.where(w, 1.0, 0.0).astype(BF16) for w in wanted)
    left = lax.broadcasted_iota(jnp.int32, (1, LANES), 1) < value_size
    o_ref[...] = jnp.zeros_like(o_ref)
    for group, at, place, pair, column, kind in tile_list(nq.shape[1], wq.shape[1], heads, value_size):
        q_ref, f_ref, r_ref = ((nq, nf, nr), (wq, wf, wr))[group]
        lanes = slice(at, at + LANES)
        out_lanes = slice(place, place + LANES)
        columns = slice(column, column + LANES)
        q = jax.nn.silu(q_ref[:, lanes].astype(F32))
        first, second = group * heads + pair[0], group * heads + pair[1]
        extra = jnp.where(left, ex[:, first : first + 1], ex[:, second : second + 1])
        values = v[:, columns]
        mask = state_mask(kind, value_size)
        scores = [None, None]
        carried = [None] * blocks
        for d in range(2):
            opening = jax.nn.sigmoid(-f_ref[d, :, lanes].astype(F32)) * r_ref[d : d + 1, lanes]
            decay = jnp.log1p(-opening) + extra
            inside = split_dot(tri[d], decay)
            query = (q * jnp.exp(inside)).astype(BF16)
            key = (opening * jnp.exp(-inside)).astype(BF16)
            for h in range(2 if kind == 2 else 1):
                own = query if kind != 2 else jnp.where(left == (h == 0), query, jnp.zeros_like(query))
                part = jnp.where(wanted[d], dot(own, key, NT), 0.0)
                scores[h] = part if scores[h] is None else scores[h] + part
            state = None
            prefix = jnp.zeros((1, LANES), F32)
            for b in range(blocks) if d == 0 else range(blocks - 1, -1, -1):
                lo = b * BLOCK
                rows = slice(lo, lo + BLOCK)
                edge = lo + BLOCK - 1 if d == 0 else lo
                ending = inside[edge : edge + 1]
                run_ref[d, rows, out_lanes] = (q[rows] * jnp.exp(prefix + inside[rows])).astype(BF16)
                if state is not None:
                    read = dot(query[rows], state.astype(BF16), NT)
                    carried[b] = read if carried[b] is None else carried[b] + read
                closing = (opening[rows] * jnp.exp(ending - inside[rows])).astype(BF16)
                added = jnp.where(mask, dot(values[rows], closing, TN), 0.0)
                state = added if state is None else state * jnp.exp(ending) + added
                prefix = prefix + ending
            msg_ref[d, :value_size, out_lanes] = (state[:value_size] + state[value_size:]).astype(BF16)
            msg_ref[d, value_size:, out_lanes] = jnp.broadcast_to(
                jnp.exp(prefix), (msg_ref.shape[1] - value_size, LANES)
            ).astype(BF16)
        reads = [dot(s.astype(BF16), values) for s in scores if s is not None]
        if kind == 2:
            within = jnp.where(left, reads[0], reads[1])
        else:
            within = jnp.where(left == (kind == 0), reads[0], 0.0)
        for b in range(blocks):
            rows = slice(b * BLOCK, b * BLOCK + BLOCK)
            total = within[rows]
            if carried[b] is not None:
                total = total + carried[b]
            o_ref[rows, columns] += total


def greet(peers):
    barrier = pltpu.get_barrier_semaphore()
    for peer in peers:
        pl.semaphore_signal(barrier, inc=1, device_id=peer, device_id_type=MESH)
    pl.semaphore_wait(barrier, len(peers))


def remote(src, dst, send, recv, peer):
    return pltpu.make_async_remote_copy(
        src_ref=src, dst_ref=dst, send_sem=send, recv_sem=recv, device_id=peer, device_id_type=MESH
    )


def join_kernel(n, heads, narrow, msg, run, o_in, gates, gain, mixed, held, send, recv):
    me = lax.axis_index("sp")
    value_size = gain.shape[1] // (2 * heads)
    greet([{"sp": lax.rem(me + d, n)} for d in range(1, n)])
    sent = []
    for d in range(1, n):
        to = lax.rem(me + d, n)
        way = jnp.where(to > me, 0, 1)
        copy = remote(msg.at[way], held.at[me], send.at[d], recv.at[me], {"sp": to})
        copy.start()
        sent.append(copy)
    for d in range(1, n):
        source = lax.rem(me + d, n)
        remote(msg.at[0], held.at[source], send.at[d], recv.at[source], {"sp": source}).wait_recv()
    channels = msg.shape[2]

    def one(source, state):
        block = held[source].astype(F32)
        return state * block[value_size : value_size + 1] + block[:value_size]

    zero = jnp.zeros((value_size, channels), F32)
    ahead = lax.fori_loop(0, me, one, zero)
    behind = lax.fori_loop(0, n - 1 - me, lambda i, s: one(n - 1 - i, s), zero)
    entering = (ahead.astype(BF16), behind.astype(BF16))
    sums = {}
    for _, _, place, _, column, kind in tile_list(narrow, channels - narrow, heads, value_size):
        lanes = slice(place, place + LANES)
        mask = state_mask(kind, value_size)
        for d in range(2):
            part = entering[d][:, lanes]
            state = jnp.where(mask, jnp.concatenate([part, part], 0), jnp.zeros((LANES, LANES), BF16))
            read = dot(run[d, :, lanes], state, NT)
            sums[column] = read if column not in sums else sums[column] + read
    ones = jnp.where(state_mask(2, value_size), 1.0, 0.0).astype(BF16)
    for column, total in sums.items():
        columns = slice(column, column + LANES)
        o = o_in[:, columns] + total
        square = o * o
        hi = square.astype(BF16)
        lo = (square - hi.astype(F32)).astype(BF16)
        scale = lax.rsqrt((dot(hi, ones) + dot(lo, ones)) / value_size + EPS)
        gate = jax.nn.silu(gates[:, columns].astype(F32))
        mixed[:, columns] = (o * scale * gain[:, columns] * gate).astype(BF16)
    for copy in sent:
        copy.wait_send()


def spread_kernel(n, x, out, send, recv, local):
    me = lax.axis_index("tp")
    own = pltpu.make_async_copy(x.at[me], out.at[me], local)
    own.start()
    greet([{"tp": lax.rem(me + d, n)} for d in range(1, n)])
    sent = []
    for d in range(1, n):
        to = lax.rem(me + d, n)
        copy = remote(x.at[to], out.at[me], send.at[d], recv.at[me], {"tp": to})
        copy.start()
        sent.append(copy)
    for d in range(1, n):
        source = lax.rem(me + d, n)
        remote(x.at[0], out.at[source], send.at[d], recv.at[source], {"tp": source}).wait_recv()
    for copy in sent:
        copy.wait_send()
    own.wait()


def tp_peers(n):
    me = lax.axis_index("tp")
    low = lax.rem(me, 2)
    sibling = me + 1 - 2 * low
    across = [lax.rem(me + 2 * d, n) for d in range(1, n // 2)]
    return me, sibling, across


def dispatch_kernel(ns, nt, own, out, s1, r1, s2, r2, s3, r3, local):
    here = lax.axis_index("sp")
    me, sibling, across = tp_peers(nt)
    mine = pltpu.make_async_copy(own.at[here], out.at[me, here], local)
    mine.start()
    greet(
        [{"sp": lax.rem(here + d, ns)} for d in range(1, ns)]
        + [{"tp": sibling}]
        + [{"tp": a} for a in across]
    )
    sent = []

    def go(copy):
        copy.start()
        sent.append(copy)

    for d in range(1, ns):
        to = lax.rem(here + d, ns)
        go(remote(own.at[to], out.at[me, here], s1.at[d], r1.at[here], {"sp": to}))

    def source_of(d):
        return lax.rem(here + ns - d, ns)

    def forward(d):
        source = source_of(d)
        for k, a in enumerate(across):
            remote(own.at[0], out.at[a, source], s2.at[k, d], r2.at[a, source], {"tp": a}).wait_recv()
            go(remote(out.at[a, source], out.at[a, source], s3.at[k + 1, d], r3.at[a, source], {"tp": sibling}))

    for d in range(ns):
        source = source_of(d)
        slot = out.at[me, source]
        if d == 0:
            mine.wait()
        else:
            remote(own.at[0], slot, s1.at[d], r1.at[source], {"sp": source}).wait_recv()
        for k, a in enumerate(across):
            go(remote(slot, slot, s2.at[k, d], r2.at[me, source], {"tp": a}))
        go(remote(slot, slot, s3.at[0, d], r3.at[me, source], {"tp": sibling}))
        if d:
            forward(d - 1)
    forward(ns - 1)
    for d in range(ns):
        source = source_of(d)
        for k, a in enumerate([me] + across):
            at = a + sibling - me
            remote(own.at[0], out.at[at, source], s3.at[k, d], r3.at[at, source], {"tp": sibling}).wait_recv()
    for copy in sent:
        copy.wait_send()


def collect_kernel(ns, nt, part, out, got1, buf2, got2, buf3, s1, r1, s2, r2, s3, r3):
    here = lax.axis_index("sp")
    me, sibling, across = tp_peers(nt)
    greet(
        [{"sp": lax.rem(here + d, ns)} for d in range(1, ns)]
        + [{"tp": sibling}]
        + [{"tp": a} for a in across]
    )
    sent = []

    def go(copy):
        copy.start()
        sent.append(copy)

    def target_of(d):
        return lax.rem(here + d, ns)

    order = list(range(1, ns)) + [0]
    for d in order:
        to = target_of(d)
        for k, a in enumerate(across + [me]):
            go(remote(part.at[a + sibling - me, to], got1.at[k, d], s1.at[k, d], r1.at[k, d], {"tp": sibling}))

    def first(d):
        to = target_of(d)
        for k, a in enumerate(across + [me]):
            remote(part.at[0, 0], got1.at[k, d], s1.at[k, d], r1.at[k, d], {"tp": sibling}).wait_recv()
            buf2[k, d] = (part[a, to].astype(F32) + got1[k, d].astype(F32)).astype(BF16)

    def second(d):
        for k, a in enumerate(across):
            go(remote(buf2.at[k, d], got2.at[k, d], s2.at[k, d], r2.at[k, d], {"tp": a}))

    def third(d):
        to = target_of(d)
        total = part[me, to].astype(F32) + got1[len(across), d].astype(F32)
        for k, a in enumerate(across):
            remote(part.at[0, 0], got2.at[k, d], s2.at[k, d], r2.at[k, d], {"tp": a}).wait_recv()
            total = total + got2[k, d].astype(F32)
        if d == 0:
            out[here] = total.astype(BF16)
        else:
            buf3[d] = total.astype(BF16)

    def fourth(d):
        if d:
            to = target_of(d)
            go(remote(buf3.at[d], out.at[here], s3.at[d], r3.at[here], {"sp": to}))

    for i in range(ns + 4):
        for lag, stage in ((0, first), (1, second), (3, third), (4, fourth)):
            if 0 <= i - lag < ns:
                stage(order[i - lag])
    for d in range(1, ns):
        source = target_of(d)
        remote(part.at[0, 0], out.at[source], s3.at[d], r3.at[source], {"sp": source}).wait_recv()
    for copy in sent:
        copy.wait_send()


def call(kernel, shapes, scratch, number, *args):
    shapes = [jax.ShapeDtypeStruct(*s) for s in shapes]
    one = len(shapes) == 1
    params = (
        dict(vmem_limit_bytes=48 * 1024 * 1024)
        if number is None
        else dict(vmem_limit_bytes=48 * 1024 * 1024, collective_id=number, has_side_effects=True)
    )
    return pl.pallas_call(
        kernel,
        out_shape=shapes[0] if one else shapes,
        in_specs=[VMEM] * len(args),
        out_specs=VMEM if one else [VMEM] * len(shapes),
        scratch_shapes=scratch,
        compiler_params=pltpu.CompilerParams(**params),
    )(*args)


def slot_table(block_routes, experts, capacity):
    flattened = block_routes.reshape(-1)
    matches = (flattened[:, None] == jnp.arange(experts, dtype=jnp.int32)[None, :]).astype(
        jnp.int32
    )
    earlier = jnp.cumsum(matches, axis=0) - matches
    token_position = jnp.sum(earlier * matches, axis=1)
    return (flattened * capacity + token_position).reshape(block_routes.shape)


def dispatch(block_slots, block_rows, slot_count):
    picks = jnp.sum(
        (block_slots[:, :, None] == jnp.arange(slot_count, dtype=jnp.int32)).astype(jnp.bfloat16),
        axis=1,
    )
    return jnp.einsum("rs,rd->sd", picks, block_rows, preferred_element_type=jnp.float32).astype(
        jnp.bfloat16
    )


def local(
    stream,
    narrow_query_weight,
    wide_query_weight,
    value_rows_heads,
    output_gate_logits,
    narrow_forget_logits,
    wide_forget_logits,
    narrow_forget_headroom,
    wide_forget_headroom,
    extra_log_decay,
    per_head_norm_gain,
    mixer_output_weight,
    feedforward_norm_gain,
    expert_gate_matrix,
    expert_up_matrix,
    expert_down_matrix,
    routes,
    router_scores_chosen,
):
    ns, nt = lax.axis_size("sp"), lax.axis_size("tp")
    token_rows, model_width = stream.shape
    heads = extra_log_decay.shape[2]
    narrow, wide = narrow_query_weight.shape[1], wide_query_weight.shape[1]
    channels = narrow + wide
    value_size = value_rows_heads.shape[2] // heads
    width = 2 * heads * value_size
    sem = pltpu.SemaphoreType.DMA
    o, run, msg = call(
        partial(mix_kernel, heads),
        [
            ((token_rows, width), F32),
            ((2, token_rows, channels), BF16),
            ((2, value_size + 16, channels), BF16),
        ],
        [],
        None,
        narrow_query_weight,
        wide_query_weight,
        value_rows_heads.reshape(token_rows, width),
        narrow_forget_logits,
        wide_forget_logits,
        narrow_forget_headroom,
        wide_forget_headroom,
        extra_log_decay.reshape(token_rows, 2 * heads),
    )
    mixed = call(
        partial(join_kernel, ns, heads, narrow),
        [((token_rows, width), BF16)],
        [pltpu.VMEM((ns,) + msg.shape[1:], BF16), sem((ns,)), sem((ns,))],
        0,
        msg,
        run,
        o,
        output_gate_logits.reshape(token_rows, width),
        jnp.tile(per_head_norm_gain, 2 * heads)[None],
    )
    row_count = token_rows // nt
    spread = call(
        partial(spread_kernel, nt),
        [((nt, row_count, width), BF16)],
        [sem((nt,)), sem((nt,)), sem],
        1,
        mixed.reshape(nt, row_count, width),
    )
    own_mixed = spread.reshape(nt, row_count, 2, -1).transpose(1, 2, 0, 3).reshape(row_count, -1)
    own_index = lax.axis_index("tp")

    def own_part(x):
        return lax.dynamic_slice_in_dim(x, own_index * row_count, row_count, 0)

    projected = jnp.dot(
        own_mixed,
        mixer_output_weight.reshape(-1, model_width),
        preferred_element_type=F32,
    )
    residual = own_part(stream).astype(F32) + projected
    norm_rows = (
        residual
        * lax.rsqrt(jnp.mean(residual * residual, axis=-1, keepdims=True) + EPS)
        * feedforward_norm_gain
    ).astype(BF16)
    top_count = routes.shape[1]
    capacity = max(2, 2 * top_count * row_count // ns)
    slot_count = ns * capacity
    own_slots = slot_table(own_part(routes), ns, capacity)
    own_buffer = dispatch(own_slots, norm_rows, slot_count).reshape(ns, capacity, model_width)
    pairs = nt // 2
    arrived = call(
        partial(dispatch_kernel, ns, nt),
        [((nt, ns, capacity, model_width), BF16)],
        [sem((ns,)), sem((ns,)), sem((pairs, ns)), sem((nt, ns)), sem((pairs, ns)), sem((nt, ns)), sem],
        2,
        own_buffer,
    ).reshape(-1, model_width)
    gate_part = jnp.dot(arrived, expert_gate_matrix[0], preferred_element_type=F32)
    up_part = jnp.dot(arrived, expert_up_matrix[0], preferred_element_type=F32)
    hidden = (jax.nn.silu(gate_part) * up_part).astype(BF16)
    part = jnp.dot(hidden, expert_down_matrix[0], preferred_element_type=F32).astype(BF16)
    block = (pairs, ns, capacity, model_width)
    returned = call(
        partial(collect_kernel, ns, nt),
        [((ns, capacity, model_width), BF16)],
        [pltpu.VMEM(block, BF16)] * 3
        + [pltpu.VMEM(block[1:], BF16)]
        + [sem((pairs, ns))] * 4
        + [sem((ns,))] * 2,
        3,
        part.reshape(nt, ns, capacity, model_width),
    )
    picked = returned.reshape(slot_count, model_width)[own_slots]
    own_logits = own_part(router_scores_chosen)
    weights = jax.nn.sigmoid(own_logits - own_logits[:, ::-1])
    mixed_out = jnp.sum(weights[:, :, None] * picked.astype(F32), axis=1)
    return (residual + mixed_out).astype(BF16)


def solution(mesh):
    placed = (
        P("sp", None),
        P("sp", "tp"),
        P("sp", "tp"),
        P("sp", None, "tp"),
        P("sp", None, "tp"),
        P(None, "sp", "tp"),
        P(None, "sp", "tp"),
        P(None, "tp"),
        P(None, "tp"),
        P("sp", None, "tp"),
        P(),
        P(),
        P(),
        P("sp", None, "tp"),
        P("sp", None, "tp"),
        P("sp", "tp", None),
        P("sp", None),
        P("sp", None),
    )
    return jax.shard_map(
        local, mesh=mesh, in_specs=placed, out_specs=P(("sp", "tp"), None), check_vma=False
    )
```

```python
from functools import partial

import jax
import jax.numpy as jnp
from jax import lax
from jax.experimental import pallas as pl
from jax.experimental.pallas import tpu as pltpu
from jax.sharding import PartitionSpec as P

BLOCK = 64
LANES = 128
EPS = 1e-06
F32 = jnp.float32
BF16 = jnp.bfloat16
MESH = pl.DeviceIdType.MESH
NT = (((1,), (1,)), ((), ()))
TN = (((0,), (0,)), ((), ()))
VMEM = pl.BlockSpec(memory_space=pltpu.VMEM)


def dot(a, b, dims=(((1,), (0,)), ((), ()))):
    return lax.dot_general(a, b, dims, preferred_element_type=F32)


def split_dot(exact, x):
    hi = x.astype(BF16)
    lo = (x - hi.astype(F32)).astype(BF16)
    return dot(exact, hi) + dot(exact, lo)


def tile_list(narrow, wide, heads, value_size):
    tiles = []
    pairs = heads * value_size // LANES
    for j in range(narrow // LANES):
        tiles.append((0, j * LANES, j * LANES, (2 * j, 2 * j + 1), j * LANES, 2))
    for h in range(wide // LANES):
        at = h * LANES
        tiles.append((1, at, narrow + at, (h, h), (pairs + h // 2) * LANES, h % 2))
    return tiles


def state_mask(kind, value_size):
    rows = lax.broadcasted_iota(jnp.int32, (LANES, LANES), 0) // value_size
    cols = lax.broadcasted_iota(jnp.int32, (LANES, LANES), 1) // value_size
    return rows == cols if kind == 2 else rows == kind


def mix_kernel(heads, nq, wq, v, nf, wf, nr, wr, ex, o_ref, run_ref, msg_ref):
    tokens = nq.shape[0]
    value_size = v.shape[1] // (2 * heads)
    blocks = tokens // BLOCK
    row = lax.broadcasted_iota(jnp.int32, (tokens, tokens), 0)
    col = lax.broadcasted_iota(jnp.int32, (tokens, tokens), 1)
    same = (row // BLOCK) == (col // BLOCK)
    wanted = (same & (row >= col), same & (row <= col))
    tri = tuple(jnp.where(w, 1.0, 0.0).astype(BF16) for w in wanted)
    left = lax.broadcasted_iota(jnp.int32, (1, LANES), 1) < value_size
    o_ref[...] = jnp.zeros_like(o_ref)
    for group, at, place, pair, column, kind in tile_list(nq.shape[1], wq.shape[1], heads, value_size):
        q_ref, f_ref, r_ref = ((nq, nf, nr), (wq, wf, wr))[group]
        lanes = slice(at, at + LANES)
        out_lanes = slice(place, place + LANES)
        columns = slice(column, column + LANES)
        q = jax.nn.silu(q_ref[:, lanes].astype(F32))
        first, second = group * heads + pair[0], group * heads + pair[1]
        extra = jnp.where(left, ex[:, first : first + 1], ex[:, second : second + 1])
        values = v[:, columns]
        mask = state_mask(kind, value_size)
        scores = [None, None]
        carried = [None] * blocks
        for d in range(2):
            opening = jax.nn.sigmoid(-f_ref[d, :, lanes].astype(F32)) * r_ref[d : d + 1, lanes]
            decay = jnp.log1p(-opening) + extra
            inside = split_dot(tri[d], decay)
            query = (q * jnp.exp(inside)).astype(BF16)
            key = (opening * jnp.exp(-inside)).astype(BF16)
            for h in range(2 if kind == 2 else 1):
                own = query if kind != 2 else jnp.where(left == (h == 0), query, jnp.zeros_like(query))
                part = jnp.where(wanted[d], dot(own, key, NT), 0.0)
                scores[h] = part if scores[h] is None else scores[h] + part
            state = None
            prefix = jnp.zeros((1, LANES), F32)
            for b in range(blocks) if d == 0 else range(blocks - 1, -1, -1):
                lo = b * BLOCK
                rows = slice(lo, lo + BLOCK)
                edge = lo + BLOCK - 1 if d == 0 else lo
                ending = inside[edge : edge + 1]
                run_ref[d, rows, out_lanes] = (q[rows] * jnp.exp(prefix + inside[rows])).astype(BF16)
                if state is not None:
                    read = dot(query[rows], state.astype(BF16), NT)
                    carried[b] = read if carried[b] is None else carried[b] + read
                closing = (opening[rows] * jnp.exp(ending - inside[rows])).astype(BF16)
                added = jnp.where(mask, dot(values[rows], closing, TN), 0.0)
                state = added if state is None else state * jnp.exp(ending) + added
                prefix = prefix + ending
            msg_ref[d, :value_size, out_lanes] = (state[:value_size] + state[value_size:]).astype(BF16)
            msg_ref[d, value_size:, out_lanes] = jnp.broadcast_to(
                jnp.exp(prefix), (msg_ref.shape[1] - value_size, LANES)
            ).astype(BF16)
        reads = [dot(s.astype(BF16), values) for s in scores if s is not None]
        if kind == 2:
            within = jnp.where(left, reads[0], reads[1])
        else:
            within = jnp.where(left == (kind == 0), reads[0], 0.0)
        for b in range(blocks):
            rows = slice(b * BLOCK, b * BLOCK + BLOCK)
            total = within[rows]
            if carried[b] is not None:
                total = total + carried[b]
            o_ref[rows, columns] += total


def partner(me, d, n):
    assert n & (n - 1) == 0
    place, bit = me, 1
    while bit < n:
        if d & bit:
            place = place + bit * (1 - 2 * lax.rem(lax.div(me, bit), 2))
        bit *= 2
    return place


def greet(peers):
    barrier = pltpu.get_barrier_semaphore()
    for peer in peers:
        pl.semaphore_signal(barrier, inc=1, device_id=peer, device_id_type=MESH)
    pl.semaphore_wait(barrier, len(peers))


def remote(src, dst, send, recv, peer):
    return pltpu.make_async_remote_copy(
        src_ref=src, dst_ref=dst, send_sem=send, recv_sem=recv, device_id=peer, device_id_type=MESH
    )


def join_kernel(n, heads, narrow, msg, run, o_in, gates, gain, mixed, held, send, recv):
    me = lax.axis_index("sp")
    value_size = gain.shape[1] // (2 * heads)
    greet([{"sp": partner(me, d, n)} for d in range(1, n)])
    sent = []
    for d in range(1, n):
        to = partner(me, d, n)
        way = jnp.where(to > me, 0, 1)
        copy = remote(msg.at[way], held.at[me], send.at[d], recv.at[me], {"sp": to})
        copy.start()
        sent.append(copy)
    for d in range(1, n):
        source = partner(me, d, n)
        remote(msg.at[0], held.at[source], send.at[d], recv.at[source], {"sp": source}).wait_recv()
    channels = msg.shape[2]

    def one(source, state):
        block = held[source].astype(F32)
        return state * block[value_size : value_size + 1] + block[:value_size]

    zero = jnp.zeros((value_size, channels), F32)
    ahead = lax.fori_loop(0, me, one, zero)
    behind = lax.fori_loop(0, n - 1 - me, lambda i, s: one(n - 1 - i, s), zero)
    entering = (ahead.astype(BF16), behind.astype(BF16))
    sums = {}
    for _, _, place, _, column, kind in tile_list(narrow, channels - narrow, heads, value_size):
        lanes = slice(place, place + LANES)
        mask = state_mask(kind, value_size)
        for d in range(2):
            part = entering[d][:, lanes]
            state = jnp.where(mask, jnp.concatenate([part, part], 0), jnp.zeros((LANES, LANES), BF16))
            read = dot(run[d, :, lanes], state, NT)
            sums[column] = read if column not in sums else sums[column] + read
    ones = jnp.where(state_mask(2, value_size), 1.0, 0.0).astype(BF16)
    for column, total in sums.items():
        columns = slice(column, column + LANES)
        o = o_in[:, columns] + total
        square = o * o
        hi = square.astype(BF16)
        lo = (square - hi.astype(F32)).astype(BF16)
        scale = lax.rsqrt((dot(hi, ones) + dot(lo, ones)) / value_size + EPS)
        gate = jax.nn.silu(gates[:, columns].astype(F32))
        mixed[:, columns] = (o * scale * gain[:, columns] * gate).astype(BF16)
    for copy in sent:
        copy.wait_send()


def spread_kernel(n, x, out, send, recv, local):
    me = lax.axis_index("tp")
    own = pltpu.make_async_copy(x.at[me], out.at[me], local)
    own.start()
    greet([{"tp": lax.rem(me + d, n)} for d in range(1, n)])
    sent = []
    for d in range(1, n):
        to = lax.rem(me + d, n)
        copy = remote(x.at[to], out.at[me], send.at[d], recv.at[me], {"tp": to})
        copy.start()
        sent.append(copy)
    for d in range(1, n):
        source = lax.rem(me + d, n)
        remote(x.at[0], out.at[source], send.at[d], recv.at[source], {"tp": source}).wait_recv()
    for copy in sent:
        copy.wait_send()
    own.wait()


def tp_peers(n):
    me = lax.axis_index("tp")
    low = lax.rem(me, 2)
    sibling = me + 1 - 2 * low
    across = [lax.rem(me + 2 * d, n) for d in range(1, n // 2)]
    return me, sibling, across


def dispatch_kernel(ns, nt, own, out, s1, r1, s2, r2, s3, r3, local):
    here = lax.axis_index("sp")
    me, sibling, across = tp_peers(nt)
    mine = pltpu.make_async_copy(own.at[here], out.at[me, here], local)
    mine.start()
    greet(
        [{"sp": partner(here, d, ns)} for d in range(1, ns)]
        + [{"tp": sibling}]
        + [{"tp": a} for a in across]
    )
    sent = []

    def go(copy):
        copy.start()
        sent.append(copy)

    for d in range(1, ns):
        to = partner(here, d, ns)
        go(remote(own.at[to], out.at[me, here], s1.at[d], r1.at[here], {"sp": to}))

    def source_of(d):
        return partner(here, d, ns)

    def forward(d):
        source = source_of(d)
        for k, a in enumerate(across):
            remote(own.at[0], out.at[a, source], s2.at[k, d], r2.at[a, source], {"tp": a}).wait_recv()
            go(remote(out.at[a, source], out.at[a, source], s3.at[k + 1, d], r3.at[a, source], {"tp": sibling}))

    for d in range(ns):
        source = source_of(d)
        slot = out.at[me, source]
        if d == 0:
            mine.wait()
        else:
            remote(own.at[0], slot, s1.at[d], r1.at[source], {"sp": source}).wait_recv()
        for k, a in enumerate(across):
            go(remote(slot, slot, s2.at[k, d], r2.at[me, source], {"tp": a}))
        go(remote(slot, slot, s3.at[0, d], r3.at[me, source], {"tp": sibling}))
        if d:
            forward(d - 1)
    forward(ns - 1)
    for d in range(ns):
        source = source_of(d)
        for k, a in enumerate([me] + across):
            at = a + sibling - me
            remote(own.at[0], out.at[at, source], s3.at[k, d], r3.at[at, source], {"tp": sibling}).wait_recv()
    for copy in sent:
        copy.wait_send()


def collect_kernel(ns, nt, part, out, got1, buf2, got2, buf3, s1, r1, s2, r2, s3, r3):
    here = lax.axis_index("sp")
    me, sibling, across = tp_peers(nt)
    greet(
        [{"sp": partner(here, d, ns)} for d in range(1, ns)]
        + [{"tp": sibling}]
        + [{"tp": a} for a in across]
    )
    sent = []

    def go(copy):
        copy.start()
        sent.append(copy)

    def target_of(d):
        return partner(here, d, ns)

    order = list(range(ns - 1, -1, -1))
    for d in order:
        to = target_of(d)
        for k, a in enumerate(across + [me]):
            go(remote(part.at[a + sibling - me, to], got1.at[k, d], s1.at[k, d], r1.at[k, d], {"tp": sibling}))

    def first(d):
        to = target_of(d)
        for k, a in enumerate(across + [me]):
            remote(part.at[0, 0], got1.at[k, d], s1.at[k, d], r1.at[k, d], {"tp": sibling}).wait_recv()
            buf2[k, d] = (part[a, to].astype(F32) + got1[k, d].astype(F32)).astype(BF16)

    def second(d):
        for k, a in enumerate(across):
            go(remote(buf2.at[k, d], got2.at[k, d], s2.at[k, d], r2.at[k, d], {"tp": a}))

    def third(d):
        to = target_of(d)
        total = part[me, to].astype(F32) + got1[len(across), d].astype(F32)
        for k, a in enumerate(across):
            remote(part.at[0, 0], got2.at[k, d], s2.at[k, d], r2.at[k, d], {"tp": a}).wait_recv()
            total = total + got2[k, d].astype(F32)
        if d == 0:
            out[here] = total.astype(BF16)
        else:
            buf3[d] = total.astype(BF16)

    def fourth(d):
        if d:
            to = target_of(d)
            go(remote(buf3.at[d], out.at[here], s3.at[d], r3.at[here], {"sp": to}))

    for i in range(ns + 4):
        for lag, stage in ((0, first), (1, second), (3, third), (4, fourth)):
            if 0 <= i - lag < ns:
                stage(order[i - lag])
    for d in range(1, ns):
        source = target_of(d)
        remote(part.at[0, 0], out.at[source], s3.at[d], r3.at[source], {"sp": source}).wait_recv()
    for copy in sent:
        copy.wait_send()


def call(kernel, shapes, scratch, number, *args):
    shapes = [jax.ShapeDtypeStruct(*s) for s in shapes]
    one = len(shapes) == 1
    params = (
        dict(vmem_limit_bytes=48 * 1024 * 1024)
        if number is None
        else dict(vmem_limit_bytes=48 * 1024 * 1024, collective_id=number, has_side_effects=True)
    )
    return pl.pallas_call(
        kernel,
        out_shape=shapes[0] if one else shapes,
        in_specs=[VMEM] * len(args),
        out_specs=VMEM if one else [VMEM] * len(shapes),
        scratch_shapes=scratch,
        compiler_params=pltpu.CompilerParams(**params),
    )(*args)


def slot_table(block_routes, experts, capacity):
    flattened = block_routes.reshape(-1)
    matches = (flattened[:, None] == jnp.arange(experts, dtype=jnp.int32)[None, :]).astype(
        jnp.int32
    )
    earlier = jnp.cumsum(matches, axis=0) - matches
    token_position = jnp.sum(earlier * matches, axis=1)
    return (flattened * capacity + token_position).reshape(block_routes.shape)


def dispatch(block_slots, block_rows, slot_count):
    picks = jnp.sum(
        (block_slots[:, :, None] == jnp.arange(slot_count, dtype=jnp.int32)).astype(jnp.bfloat16),
        axis=1,
    )
    return jnp.einsum("rs,rd->sd", picks, block_rows, preferred_element_type=jnp.float32).astype(
        jnp.bfloat16
    )


def local(
    stream,
    narrow_query_weight,
    wide_query_weight,
    value_rows_heads,
    output_gate_logits,
    narrow_forget_logits,
    wide_forget_logits,
    narrow_forget_headroom,
    wide_forget_headroom,
    extra_log_decay,
    per_head_norm_gain,
    mixer_output_weight,
    feedforward_norm_gain,
    expert_gate_matrix,
    expert_up_matrix,
    expert_down_matrix,
    routes,
    router_scores_chosen,
):
    ns, nt = lax.axis_size("sp"), lax.axis_size("tp")
    token_rows, model_width = stream.shape
    heads = extra_log_decay.shape[2]
    narrow, wide = narrow_query_weight.shape[1], wide_query_weight.shape[1]
    channels = narrow + wide
    value_size = value_rows_heads.shape[2] // heads
    width = 2 * heads * value_size
    sem = pltpu.SemaphoreType.DMA
    o, run, msg = call(
        partial(mix_kernel, heads),
        [
            ((token_rows, width), F32),
            ((2, token_rows, channels), BF16),
            ((2, value_size + 16, channels), BF16),
        ],
        [],
        None,
        narrow_query_weight,
        wide_query_weight,
        value_rows_heads.reshape(token_rows, width),
        narrow_forget_logits,
        wide_forget_logits,
        narrow_forget_headroom,
        wide_forget_headroom,
        extra_log_decay.reshape(token_rows, 2 * heads),
    )
    mixed = call(
        partial(join_kernel, ns, heads, narrow),
        [((token_rows, width), BF16)],
        [pltpu.VMEM((ns,) + msg.shape[1:], BF16), sem((ns,)), sem((ns,))],
        0,
        msg,
        run,
        o,
        output_gate_logits.reshape(token_rows, width),
        jnp.tile(per_head_norm_gain, 2 * heads)[None],
    )
    row_count = token_rows // nt
    spread = call(
        partial(spread_kernel, nt),
        [((nt, row_count, width), BF16)],
        [sem((nt,)), sem((nt,)), sem],
        1,
        mixed.reshape(nt, row_count, width),
    )
    own_mixed = spread.reshape(nt, row_count, 2, -1).transpose(1, 2, 0, 3).reshape(row_count, -1)
    own_index = lax.axis_index("tp")

    def own_part(x):
        return lax.dynamic_slice_in_dim(x, own_index * row_count, row_count, 0)

    projected = jnp.dot(
        own_mixed,
        mixer_output_weight.reshape(-1, model_width),
        preferred_element_type=F32,
    )
    residual = own_part(stream).astype(F32) + projected
    norm_rows = (
        residual
        * lax.rsqrt(jnp.mean(residual * residual, axis=-1, keepdims=True) + EPS)
        * feedforward_norm_gain
    ).astype(BF16)
    top_count = routes.shape[1]
    capacity = max(2, 2 * top_count * row_count // ns)
    slot_count = ns * capacity
    own_slots = slot_table(own_part(routes), ns, capacity)
    own_buffer = dispatch(own_slots, norm_rows, slot_count).reshape(ns, capacity, model_width)
    pairs = nt // 2
    arrived = call(
        partial(dispatch_kernel, ns, nt),
        [((nt, ns, capacity, model_width), BF16)],
        [sem((ns,)), sem((ns,)), sem((pairs, ns)), sem((nt, ns)), sem((pairs, ns)), sem((nt, ns)), sem],
        2,
        own_buffer,
    ).reshape(-1, model_width)
    gate_part = jnp.dot(arrived, expert_gate_matrix[0], preferred_element_type=F32)
    up_part = jnp.dot(arrived, expert_up_matrix[0], preferred_element_type=F32)
    hidden = (jax.nn.silu(gate_part) * up_part).astype(BF16)
    part = jnp.dot(hidden, expert_down_matrix[0], preferred_element_type=F32).astype(BF16)
    block = (pairs, ns, capacity, model_width)
    returned = call(
        partial(collect_kernel, ns, nt),
        [((ns, capacity, model_width), BF16)],
        [pltpu.VMEM(block, BF16)] * 3
        + [pltpu.VMEM(block[1:], BF16)]
        + [sem((pairs, ns))] * 4
        + [sem((ns,))] * 2,
        3,
        part.reshape(nt, ns, capacity, model_width),
    )
    picked = returned.reshape(slot_count, model_width)[own_slots]
    own_logits = own_part(router_scores_chosen)
    weights = jax.nn.sigmoid(own_logits - own_logits[:, ::-1])
    mixed_out = jnp.sum(weights[:, :, None] * picked.astype(F32), axis=1)
    return (residual + mixed_out).astype(BF16)


def solution(mesh):
    placed = (
        P("sp", None),
        P("sp", "tp"),
        P("sp", "tp"),
        P("sp", None, "tp"),
        P("sp", None, "tp"),
        P(None, "sp", "tp"),
        P(None, "sp", "tp"),
        P(None, "tp"),
        P(None, "tp"),
        P("sp", None, "tp"),
        P(),
        P(),
        P(),
        P("sp", None, "tp"),
        P("sp", None, "tp"),
        P("sp", "tp", None),
        P("sp", None),
        P("sp", None),
    )
    return jax.shard_map(
        local, mesh=mesh, in_specs=placed, out_specs=P(("sp", "tp"), None), check_vma=False
    )
```
